32 devices in a mesh: sp: 16 (over z, y, x), tp: 2 (over core).
Axes of the slice: x: 2, y: 2, z: 4, core: 2. Of those that a mesh axis runs over, the one named last changes fastest.
Arguments:
- queries: bfloat16 [8192, 2048], P('sp', 'tp'), may hold values from -6 to 6
- key_rows: bfloat16 [8192, 512], P('sp', 'tp'), may hold values from -6 to 6
- values: bfloat16 [8192, 512], P('sp', 'tp'), may hold values from -6 to 6
- sink_logit: float32 [32], P('tp'), may hold values from 4 to 10
- residual_in: bfloat16 [8192, 2048], P(('sp', 'tp')), may hold values from -6 to 6
- out_weight: bfloat16 [2048, 2048], P('tp'), may hold values from -0.125 to 0.125
- norm_gain: float32 [2048], replicated, may hold values from 0.1 to 1.9
- gate_weight: bfloat16 [2048, 5632], P('sp', 'tp'), may hold values from -0.125 to 0.125
- up_weight: bfloat16 [2048, 5632], P('sp', 'tp'), may hold values from -0.125 to 0.125
- down_weight: bfloat16 [5632, 2048], P('tp', 'sp'), may hold values from -0.078125 to 0.078125
Outputs:
- layer_out: bfloat16 [8192, 2048], P(('sp', 'tp'))
The draws below stay inside these ranges and needn't reach their ends.
All inputs are finite; a program needn't handle non-finite values.
Results may differ from the reference program's by a relative error of at most 0.013.
Values may be sent and summed in bfloat16 or wider, within the bound.
A program may use at most 128 MiB of HBM per device.

```python
import jax
import jax.numpy as jnp
from jax import lax

D = 2048
HEADS = 32
KV_HEADS = 8
HEAD_DIM = 64
FF = 5632
WINDOW = 128
TOK_DEV = 512
TOKENS = 8192
N_TP = 2


def base_draw(key, columns):
    return jnp.clip(1.7 * jax.random.normal(key, (TOKENS, columns), jnp.float32), -6.0, 6.0)


def draw_queries(key, part):
    result = base_draw(jax.random.fold_in(key, 1), HEADS * HEAD_DIM)
    return result.astype(jnp.bfloat16)


def draw_key_rows(key, part):
    result = base_draw(jax.random.fold_in(key, 2), KV_HEADS * HEAD_DIM)
    return result.astype(jnp.bfloat16)


def level_of(stream_key, dims, split, least, high):
    loudness, own = 1.0, jax.random.fold_in(stream_key, 6)
    for dim, shards_of in split:
        steps = jnp.exp(jax.random.uniform(jax.random.fold_in(own, dim), (shards_of,), jnp.float32, least / len(split), high / len(split)))
        loudness = loudness * jnp.repeat(steps, dims[dim] // shards_of).reshape([-1 if axis == dim else 1 for axis in range(len(dims))])
    return loudness


def scatter_about(rng, dims, spread, limit, shards=(), kind=jnp.bfloat16):
    values = jax.random.normal(rng, dims, jnp.float32) * spread
    if len(shards) > 0:
        values = level_of(rng, dims, shards, -0.22, 0.18) * values
    return jnp.clip(values, min=-limit, max=limit).astype(kind)


def setup_inputs(seed: int = 0) -> dict:
    key_list = jax.random.split(jax.random.key(seed), 11)
    return {
        "queries": draw_queries(jax.random.fold_in(key_list[10], 71), 0),
        "key_rows": draw_key_rows(jax.random.fold_in(key_list[10], 71), 0),
        "values": scatter_about(key_list[2], (TOKENS, KV_HEADS * HEAD_DIM), 1.0, 6.0, ((0, 16), (1, 2))),
        "sink_logit": jnp.clip(4.0 + 6.0 * jax.random.uniform(key_list[3], (HEADS,), jnp.float32) ** level_of(key_list[3], (HEADS,), ((0, 2),), -0.2, 0.2), 4.0, 10.0),
        "residual_in": scatter_about(key_list[4], (TOKENS, D), 1.0, 6.0, ((0, 32),)),
        "out_weight": scatter_about(key_list[5], (HEADS * HEAD_DIM, D), (HEADS * HEAD_DIM) ** -0.5, 0.125, ((0, 2),)),
        "norm_gain": jnp.clip(1.0 + 0.18 * jax.random.normal(key_list[6], (D,), jnp.float32), 0.1, 1.9),
        "gate_weight": scatter_about(key_list[7], (D, FF), D ** -0.5, 0.125, ((0, 16), (1, 2))),
        "up_weight": scatter_about(key_list[8], (D, FF), D ** -0.5, 0.125, ((0, 16), (1, 2))),
        "down_weight": scatter_about(key_list[9], (FF, D), FF ** -0.5, 0.078125, ((0, 2), (1, 16))),
    }


def rms_scale(mixed_rows, norm_gain):
    inverse = lax.rsqrt(lax.optimization_barrier(jnp.mean(mixed_rows * mixed_rows, axis=-1, keepdims=True)) + 1e-06)
    return (mixed_rows * inverse * norm_gain).astype(jnp.bfloat16)

def rounded_sum(left, right, parts):
    columns = left.shape[1] // parts
    summed = jnp.zeros((left.shape[0], right.shape[1]), jnp.float32)
    for part_index in range(parts):
        partial_value = jnp.dot(left[:, part_index * columns:(part_index + 1) * columns], right[part_index * columns:(part_index + 1) * columns], preferred_element_type=jnp.float32)
        summed = summed + lax.optimization_barrier(partial_value.astype(jnp.bfloat16)).astype(jnp.float32)
    return summed

def reference(queries, key_rows, values, sink_logit, residual_in, out_weight, norm_gain, gate_weight, up_weight, down_weight):
    group_size = HEADS // KV_HEADS
    score_scale = HEAD_DIM ** (-0.5)
    block_count = TOKENS // WINDOW
    zero_rows = jnp.zeros((WINDOW, KV_HEADS * HEAD_DIM), jnp.bfloat16)
    key_padded = jnp.concatenate([zero_rows, key_rows, zero_rows], axis=0)
    value_padded = jnp.concatenate([zero_rows, values, zero_rows], axis=0)
    sink_grid = sink_logit.astype(jnp.float32).reshape(KV_HEADS, group_size)[:, :, None, None]

    def one_block(block_index):
        start_row = (block_index * WINDOW).astype(jnp.int32)
        query_block = lax.dynamic_slice_in_dim(queries, start_row, WINDOW, 0).astype(jnp.float32)
        query_block = query_block.reshape(WINDOW, KV_HEADS, group_size, HEAD_DIM)
        key_block = lax.dynamic_slice_in_dim(key_padded, start_row, 3 * WINDOW, 0).astype(jnp.float32)
        key_block = key_block.reshape(3 * WINDOW, KV_HEADS, HEAD_DIM)
        value_block = lax.dynamic_slice_in_dim(value_padded, start_row, 3 * WINDOW, 0).astype(jnp.float32)
        value_block = value_block.reshape(3 * WINDOW, KV_HEADS, HEAD_DIM)
        scores = jnp.einsum('qkgd,skd->kgqs', query_block, key_block) * score_scale
        query_pos = start_row + jnp.arange(WINDOW, dtype=jnp.int32)
        key_pos = start_row - WINDOW + jnp.arange(3 * WINDOW, dtype=jnp.int32)
        valid = (jnp.abs(query_pos[:, None] - key_pos[None, :]) <= WINDOW) & (key_pos >= 0)[None, :] & (key_pos < TOKENS)[None, :]
        scores = jnp.where(valid, scores, -1e+30)
        peak = jnp.maximum(lax.optimization_barrier(jnp.max(scores, axis=-1, keepdims=True)), sink_grid)
        weights_raw = jnp.exp(scores - peak)
        denom = lax.optimization_barrier(jnp.sum(weights_raw, axis=-1, keepdims=True)) + jnp.exp(sink_grid - peak)
        probs = lax.optimization_barrier((weights_raw / denom).astype(jnp.bfloat16)).astype(jnp.float32)
        output = jnp.einsum('kgqs,skd->qkgd', probs, value_block).astype(jnp.bfloat16)
        return output.reshape(WINDOW, HEADS * HEAD_DIM)
    attended = lax.map(one_block, jnp.arange(block_count, dtype=jnp.int32)).reshape(TOKENS, HEADS * HEAD_DIM)
    attn_sum = rounded_sum(attended, out_weight, N_TP)
    mixed_rows = residual_in.astype(jnp.float32) + attn_sum

    def feed_forward(mixed_block):
        normed = rms_scale(mixed_block, norm_gain)
        gate_pre = jnp.dot(normed, gate_weight, preferred_element_type=jnp.float32)
        up_pre = jnp.dot(normed, up_weight, preferred_element_type=jnp.float32)
        hidden = (jax.nn.silu(gate_pre) * up_pre).astype(jnp.bfloat16)
        ffn_sum = rounded_sum(hidden, down_weight, N_TP)
        return (mixed_block + ffn_sum).astype(jnp.bfloat16)
    blocked = mixed_rows.reshape(TOKENS // TOK_DEV, TOK_DEV, D)
    return lax.map(feed_forward, blocked).reshape(TOKENS, D)
```

```python
import math

import jax
import jax.numpy as jnp
from jax import lax
from jax.sharding import Mesh
from jax.sharding import PartitionSpec as P

HEAD_DIM = 64
WINDOW = 128


def with_halo(block, sides, width):
    for axis, dim in sides:
        count = math.prod(lax.axis_size(name) for name in axis)
        forward = [(i, i + 1) for i in range(count - 1)]
        backward = [(target, source) for source, target in forward]
        low = lax.ppermute(
            lax.slice_in_dim(block, block.shape[dim] - width, None, axis=dim), axis, forward
        )
        high = lax.ppermute(lax.slice_in_dim(block, 0, width, axis=dim), axis, backward)
        block = jnp.concatenate([low, block, high], axis=dim)
    return block


def rms_scale(mixed_rows, norm_gain):
    inverse = lax.rsqrt(jnp.mean(mixed_rows * mixed_rows, axis=-1, keepdims=True) + 1e-06)
    return (mixed_rows * inverse * norm_gain).astype(jnp.bfloat16)


def attend_window(queries, padded, offset, total_rows, sink_logit):
    rows_here = queries.shape[0]
    block_count = rows_here // WINDOW
    heads_here = queries.shape[1] // HEAD_DIM
    kv_here = padded.shape[1] // (2 * HEAD_DIM)
    group_size = heads_here // kv_here
    blocks = padded.reshape(block_count + 2, WINDOW, padded.shape[1])
    banded = jnp.concatenate([blocks[:-2], blocks[1:-1], blocks[2:]], axis=1)
    key_band = banded[:, :, : kv_here * HEAD_DIM].reshape(
        block_count, 3 * WINDOW, kv_here, HEAD_DIM
    )
    value_band = banded[:, :, kv_here * HEAD_DIM :].reshape(
        block_count, 3 * WINDOW, kv_here, HEAD_DIM
    )
    grouped = queries.reshape(block_count, WINDOW, kv_here, group_size, HEAD_DIM)
    scores = jnp.einsum(
        "nqkgd,nskd->nkgqs", grouped, key_band, preferred_element_type=jnp.float32
    ) * HEAD_DIM ** (-0.5)
    block_start = offset + jnp.arange(block_count, dtype=jnp.int32)[:, None] * WINDOW
    query_pos = block_start + jnp.arange(WINDOW, dtype=jnp.int32)[None, :]
    key_pos = block_start - WINDOW + jnp.arange(3 * WINDOW, dtype=jnp.int32)[None, :]
    valid = jnp.abs(query_pos[:, :, None] - key_pos[:, None, :]) <= WINDOW
    valid = valid & ((key_pos >= 0) & (key_pos < total_rows))[:, None, :]
    scores = jnp.where(valid[:, None, None], scores, -1e30)
    sink_grid = sink_logit.reshape(kv_here, group_size)[None, :, :, None, None]
    peak = jnp.maximum(jnp.max(scores, axis=-1, keepdims=True), sink_grid)
    weights_raw = jnp.exp(scores - peak)
    denom = jnp.sum(weights_raw, axis=-1, keepdims=True) + jnp.exp(sink_grid - peak)
    probs = (weights_raw / denom).astype(jnp.bfloat16)
    output = jnp.einsum("nkgqs,nskd->nqkgd", probs, value_band, preferred_element_type=jnp.float32)
    return output.astype(jnp.bfloat16).reshape(rows_here, heads_here * HEAD_DIM)


def swap(array, axis, distance):
    count = lax.axis_size(axis)
    return lax.ppermute(array, axis, [(i, i ^ distance) for i in range(count)])


def piece(array, index, size, dim):
    return lax.dynamic_slice_in_dim(array, index * size, size, dim)


def shards(
    queries,
    key_rows,
    values,
    sink_logit,
    residual_in,
    out_weight,
    norm_gain,
    gate_weight,
    up_weight,
    down_weight,
):
    rows_here = queries.shape[0]
    tp_count, group = lax.axis_size("tp"), lax.axis_size("q")
    row_share = rows_here // tp_count
    q_index, tp_index = lax.axis_index("q"), lax.axis_index("tp")
    units = gate_weight.shape[1] // group

    joined = jnp.concatenate([key_rows, values], axis=1)
    padded = with_halo(joined, ((("o", "q"), 0),), WINDOW)

    gate_up = jnp.stack([gate_weight, up_weight])
    gate_up_got, down_got = [], []
    for k in range(group):
        part = piece(gate_up, q_index ^ k, units, 2)
        gate_up_got.append(swap(part, "q", k) if k else part)
    for k in range(group):
        part = piece(down_weight, q_index ^ k, units, 0)
        down_got.append(swap(part, "q", k) if k else part)
    depth, width = gate_weight.shape[0], down_weight.shape[1]
    gate_up_mine = jnp.zeros((2, group * depth, units), gate_weight.dtype)
    down_mine = jnp.zeros((units, group * width), down_weight.dtype)
    for k in range(group):
        gate_up_mine = lax.dynamic_update_slice_in_dim(
            gate_up_mine, gate_up_got[k], (q_index ^ k) * depth, 1
        )
        down_mine = lax.dynamic_update_slice_in_dim(
            down_mine, down_got[k], (q_index ^ k) * width, 1
        )
    gate_full = lax.all_gather(gate_up_mine[0], "o", axis=0, tiled=True)
    up_full = lax.all_gather(gate_up_mine[1], "o", axis=0, tiled=True)
    down_full = lax.all_gather(down_mine, "o", axis=1, tiled=True)

    sp_index = lax.axis_index(("o", "q"))
    total_rows = rows_here * lax.axis_size(("o", "q"))
    attended = attend_window(queries, padded, sp_index * rows_here, total_rows, sink_logit)
    partial_value = jnp.dot(attended, out_weight, preferred_element_type=jnp.float32).astype(
        jnp.bfloat16
    )
    mixed = residual_in.astype(jnp.float32) + piece(partial_value, tp_index, row_share, 0).astype(
        jnp.float32
    )
    for j in range(1, tp_count):
        sent = piece(partial_value, tp_index ^ j, row_share, 0)
        mixed = mixed + swap(sent, "tp", j).astype(jnp.float32)
    normed = rms_scale(mixed, norm_gain)

    arrived = [swap(normed, "q", k) if k else normed for k in range(group)]
    result = mixed
    for k in [*range(1, group), 0]:
        rows = jnp.concatenate(
            [swap(arrived[k], "tp", j) if j else arrived[k] for j in range(tp_count)], axis=0
        )
        gate_pre = jnp.dot(rows, gate_full, preferred_element_type=jnp.float32)
        up_pre = jnp.dot(rows, up_full, preferred_element_type=jnp.float32)
        hidden = (jax.nn.silu(gate_pre) * up_pre).astype(jnp.bfloat16)
        out = jnp.dot(hidden, down_full, preferred_element_type=jnp.float32).astype(jnp.bfloat16)
        mine = out[:row_share].astype(jnp.float32)
        for j in range(1, tp_count):
            sent = out[j * row_share : (j + 1) * row_share]
            mine = mine + swap(sent, "tp", j).astype(jnp.float32)
        if k:
            mine = swap(mine.astype(jnp.bfloat16), "q", k).astype(jnp.float32)
        result = result + mine
    return result.astype(jnp.bfloat16)


def solution(mesh):
    sp_count, tp_count = mesh.shape["sp"], mesh.shape["tp"]
    group = math.gcd(sp_count, 4)
    fine = Mesh(mesh.devices.reshape(sp_count // group, group, tp_count), ("o", "q", "tp"))
    sp = ("o", "q")
    return jax.shard_map(
        shards,
        mesh=fine,
        in_specs=(
            P(sp, "tp"),
            P(sp, "tp"),
            P(sp, "tp"),
            P("tp"),
            P(("o", "q", "tp"), None),
            P("tp", None),
            P(),
            P(sp, "tp"),
            P(sp, "tp"),
            P("tp", sp),
        ),
        out_specs=P(("o", "q", "tp"), None),
        check_vma=False,
    )
```

```python
import math

import jax
import jax.numpy as jnp
from jax import lax
from jax.sharding import Mesh
from jax.sharding import PartitionSpec as P

HEAD_DIM = 64
WINDOW = 128


def with_halo(block, sides, width):
    for axis, dim in sides:
        count = math.prod(lax.axis_size(name) for name in axis)
        forward = [(i, i + 1) for i in range(count - 1)]
        backward = [(target, source) for source, target in forward]
        low = lax.ppermute(
            lax.slice_in_dim(block, block.shape[dim] - width, None, axis=dim), axis, forward
        )
        high = lax.ppermute(lax.slice_in_dim(block, 0, width, axis=dim), axis, backward)
        block = jnp.concatenate([low, block, high], axis=dim)
    return block


def rms_scale(mixed_rows, norm_gain):
    inverse = lax.rsqrt(jnp.mean(mixed_rows * mixed_rows, axis=-1, keepdims=True) + 1e-06)
    return (mixed_rows * inverse * norm_gain).astype(jnp.bfloat16)


def attend_window(queries, padded, offset, total_rows, sink_logit, between):
    rows_here = queries.shape[0]
    block_count = rows_here // WINDOW
    heads_here = queries.shape[1] // HEAD_DIM
    kv_here = padded.shape[1] // (2 * HEAD_DIM)
    group_size = heads_here // kv_here
    blocks = padded.reshape(block_count + 2, WINDOW, padded.shape[1])
    banded = jnp.concatenate([blocks[:-2], blocks[1:-1], blocks[2:]], axis=1)
    key_band = banded[:, :, : kv_here * HEAD_DIM].reshape(
        block_count, 3 * WINDOW, kv_here, HEAD_DIM
    )
    value_band = banded[:, :, kv_here * HEAD_DIM :].reshape(
        block_count, 3 * WINDOW, kv_here, HEAD_DIM
    )
    grouped = queries.reshape(block_count, WINDOW, kv_here, group_size, HEAD_DIM)
    scores = jnp.einsum(
        "nqkgd,nskd->nkgqs", grouped, key_band, preferred_element_type=jnp.float32
    ) * HEAD_DIM ** (-0.5)
    scores, moved = lax.optimization_barrier((scores, between))
    block_start = offset + jnp.arange(block_count, dtype=jnp.int32)[:, None] * WINDOW
    query_pos = block_start + jnp.arange(WINDOW, dtype=jnp.int32)[None, :]
    key_pos = block_start - WINDOW + jnp.arange(3 * WINDOW, dtype=jnp.int32)[None, :]
    valid = jnp.abs(query_pos[:, :, None] - key_pos[:, None, :]) <= WINDOW
    valid = valid & ((key_pos >= 0) & (key_pos < total_rows))[:, None, :]
    scores = jnp.where(valid[:, None, None], scores, -1e30)
    sink_grid = sink_logit.reshape(kv_here, group_size)[None, :, :, None, None]
    peak = jnp.maximum(jnp.max(scores, axis=-1, keepdims=True), sink_grid)
    weights_raw = jnp.exp(scores - peak)
    denom = jnp.sum(weights_raw, axis=-1, keepdims=True) + jnp.exp(sink_grid - peak)
    probs = (weights_raw / denom).astype(jnp.bfloat16)
    output = jnp.einsum("nkgqs,nskd->nqkgd", probs, value_band, preferred_element_type=jnp.float32)
    return output.astype(jnp.bfloat16).reshape(rows_here, heads_here * HEAD_DIM), moved


def swap(array, axis, distance):
    count = lax.axis_size(axis)
    return lax.ppermute(array, axis, [(i, i ^ distance) for i in range(count)])


def turn(array, step):
    count = lax.axis_size("o")
    return lax.ppermute(array, "o", [(i, (i + step) % count) for i in range(count)])


def piece(array, index, size, dim):
    return lax.dynamic_slice_in_dim(array, index * size, size, dim)


def shards(
    queries,
    key_rows,
    values,
    sink_logit,
    residual_in,
    out_weight,
    norm_gain,
    gate_weight,
    up_weight,
    down_weight,
):
    rows_here = queries.shape[0]
    tp_count, group = lax.axis_size("tp"), lax.axis_size("q")
    row_share = rows_here // tp_count
    q_index, tp_index = lax.axis_index("q"), lax.axis_index("tp")
    units = gate_weight.shape[1] // group

    joined = jnp.concatenate([key_rows, values], axis=1)
    padded = with_halo(joined, ((("o", "q"), 0),), WINDOW)

    gate_up = jnp.stack([gate_weight, up_weight])
    gate_up_got, down_got = [], []
    for k in range(group):
        part = piece(gate_up, q_index ^ k, units, 2)
        gate_up_got.append(swap(part, "q", k) if k else part)
    for k in range(group):
        part = piece(down_weight, q_index ^ k, units, 0)
        down_got.append(swap(part, "q", k) if k else part)
    depth, width = gate_weight.shape[0], down_weight.shape[1]
    gate_up_mine = jnp.zeros((2, group * depth, units), gate_weight.dtype)
    down_mine = jnp.zeros((units, group * width), down_weight.dtype)
    for k in range(group):
        gate_up_mine = lax.dynamic_update_slice_in_dim(
            gate_up_mine, gate_up_got[k], (q_index ^ k) * depth, 1
        )
        down_mine = lax.dynamic_update_slice_in_dim(
            down_mine, down_got[k], (q_index ^ k) * width, 1
        )
    sp_index = lax.axis_index(("o", "q"))
    total_rows = rows_here * lax.axis_size(("o", "q"))
    mine = (gate_up_mine[0], gate_up_mine[1], down_mine)
    attended, mine = attend_window(
        queries, padded, sp_index * rows_here, total_rows, sink_logit, mine
    )
    outer = lax.axis_size("o")
    pieces = [(0, mine)]
    rings = [(x, x) for x in mine]
    if outer > 2:
        rings = [(turn(x, 1), turn(x, -1)) for x in mine]
        attended, rings[0] = lax.optimization_barrier((attended, rings[0]))

    partial_value = jnp.dot(attended, out_weight, preferred_element_type=jnp.float32).astype(
        jnp.bfloat16
    )
    mixed = residual_in.astype(jnp.float32) + piece(partial_value, tp_index, row_share, 0).astype(
        jnp.float32
    )
    for j in range(1, tp_count):
        sent = piece(partial_value, tp_index ^ j, row_share, 0)
        mixed = mixed + swap(sent, "tp", j).astype(jnp.float32)
    normed = rms_scale(mixed, norm_gain)

    own = normed
    if outer > 2:
        own, rings[1] = lax.optimization_barrier((normed, rings[1]))
        pieces += [(-1, [x for x, _ in rings]), (1, [y for _, y in rings])]
    for distance in range(2, (outer - 1) // 2 + 1):
        rings = [(turn(x, 1), turn(y, -1)) for x, y in rings]
        pieces += [(-distance, [x for x, _ in rings]), (distance, [y for _, y in rings])]
    if outer > 1 and outer % 2 == 0:
        far = []
        for x, y in rings:
            half = x.shape[0] // 2
            far.append(jnp.concatenate([turn(x[:half], 1), turn(y[half:], -1)], axis=0))
        pieces.append((outer // 2, far))
    gate_full = jnp.zeros((outer * group * depth, units), gate_weight.dtype)
    up_full = jnp.zeros((outer * group * depth, units), gate_weight.dtype)
    down_full = jnp.zeros((units, outer * group * width), down_weight.dtype)
    for distance, (gate_part, up_part, down_part) in pieces:
        place = lax.rem(lax.axis_index("o") + distance + outer, outer)
        row = place * group * depth
        gate_full = lax.dynamic_update_slice_in_dim(gate_full, gate_part, row, 0)
        up_full = lax.dynamic_update_slice_in_dim(up_full, up_part, row, 0)
        down_full = lax.dynamic_update_slice_in_dim(down_full, down_part, place * group * width, 1)

    order = [*range(group - 1, 0, -1), 0]
    arrived = {k: swap(normed, "q", k) for k in order if k}
    arrived[0] = own
    result = mixed
    waiting, received = None, []
    for k in order:
        rows = jnp.concatenate(
            [swap(arrived[k], "tp", j) if j else arrived[k] for j in range(tp_count)], axis=0
        )
        gate_pre = jnp.dot(rows, gate_full, preferred_element_type=jnp.float32)
        up_pre = jnp.dot(rows, up_full, preferred_element_type=jnp.float32)
        hidden = (jax.nn.silu(gate_pre) * up_pre).astype(jnp.bfloat16)
        if waiting is not None:
            sent, hidden = lax.optimization_barrier((waiting[1], hidden))
            received.append(swap(sent, "q", waiting[0]))
        if k == 0 and len(received) > 2:
            received[0], hidden = lax.optimization_barrier((received[0], hidden))
        parts = []
        for j in [*range(1, tp_count), 0]:
            if j == k == 0 and len(received) > 2:
                received[1], parts, hidden = lax.optimization_barrier(
                    (received[1], parts, hidden)
                )
            share = hidden[j * row_share : (j + 1) * row_share]
            out = jnp.dot(share, down_full, preferred_element_type=jnp.float32)
            out = out.astype(jnp.bfloat16)
            parts.append(swap(out, "tp", j) if j else out)
        total = sum(part.astype(jnp.float32) for part in parts)
        if k:
            waiting = (k, total.astype(jnp.bfloat16))
        else:
            result = result + total
    for part in received:
        result = result + part.astype(jnp.float32)
    return result.astype(jnp.bfloat16)


def solution(mesh):
    sp_count, tp_count = mesh.shape["sp"], mesh.shape["tp"]
    group = math.gcd(sp_count, 4)
    fine = Mesh(mesh.devices.reshape(sp_count // group, group, tp_count), ("o", "q", "tp"))
    sp = ("o", "q")
    return jax.shard_map(
        shards,
        mesh=fine,
        in_specs=(
            P(sp, "tp"),
            P(sp, "tp"),
            P(sp, "tp"),
            P("tp"),
            P(("o", "q", "tp"), None),
            P("tp", None),
            P(),
            P(sp, "tp"),
            P(sp, "tp"),
            P("tp", sp),
        ),
        out_specs=P(("o", "q", "tp"), None),
        check_vma=False,
    )
```

```python
import math

import jax
import jax.numpy as jnp
from jax import lax
from jax.sharding import Mesh
from jax.sharding import PartitionSpec as P

HEAD_DIM = 64
WINDOW = 128


def with_halo(block, sides, width):
    for axis, dim in sides:
        count = math.prod(lax.axis_size(name) for name in axis)
        forward = [(i, i + 1) for i in range(count - 1)]
        backward = [(target, source) for source, target in forward]
        low = lax.ppermute(
            lax.slice_in_dim(block, block.shape[dim] - width, None, axis=dim), axis, forward
        )
        high = lax.ppermute(lax.slice_in_dim(block, 0, width, axis=dim), axis, backward)
        block = jnp.concatenate([low, block, high], axis=dim)
    return block


def rms_scale(mixed_rows, norm_gain):
    inverse = lax.rsqrt(jnp.mean(mixed_rows * mixed_rows, axis=-1, keepdims=True) + 1e-06)
    return (mixed_rows * inverse * norm_gain).astype(jnp.bfloat16)


def attend_window(queries, padded, offset, total_rows, sink_logit, between):
    rows_here = queries.shape[0]
    block_count = rows_here // WINDOW
    heads_here = queries.shape[1] // HEAD_DIM
    kv_here = padded.shape[1] // (2 * HEAD_DIM)
    group_size = heads_here // kv_here
    blocks = padded.reshape(block_count + 2, WINDOW, padded.shape[1])
    banded = jnp.concatenate([blocks[:-2], blocks[1:-1], blocks[2:]], axis=1)
    key_band = banded[:, :, : kv_here * HEAD_DIM].reshape(
        block_count, 3 * WINDOW, kv_here, HEAD_DIM
    )
    value_band = banded[:, :, kv_here * HEAD_DIM :].reshape(
        block_count, 3 * WINDOW, kv_here, HEAD_DIM
    )
    grouped = queries.reshape(block_count, WINDOW, kv_here, group_size, HEAD_DIM)
    scores = jnp.einsum(
        "nqkgd,nskd->nkgqs", grouped, key_band, preferred_element_type=jnp.float32
    ) * HEAD_DIM ** (-0.5)
    scores, moved = lax.optimization_barrier((scores, between))
    block_start = offset + jnp.arange(block_count, dtype=jnp.int32)[:, None] * WINDOW
    query_pos = block_start + jnp.arange(WINDOW, dtype=jnp.int32)[None, :]
    key_pos = block_start - WINDOW + jnp.arange(3 * WINDOW, dtype=jnp.int32)[None, :]
    valid = jnp.abs(query_pos[:, :, None] - key_pos[:, None, :]) <= WINDOW
    valid = valid & ((key_pos >= 0) & (key_pos < total_rows))[:, None, :]
    scores = jnp.where(valid[:, None, None], scores, -1e30)
    sink_grid = sink_logit.reshape(kv_here, group_size)[None, :, :, None, None]
    peak = jnp.maximum(jnp.max(scores, axis=-1, keepdims=True), sink_grid)
    weights_raw = jnp.exp(scores - peak)
    denom = jnp.sum(weights_raw, axis=-1, keepdims=True) + jnp.exp(sink_grid - peak)
    probs = (weights_raw / denom).astype(jnp.bfloat16)
    output = jnp.einsum("nkgqs,nskd->nqkgd", probs, value_band, preferred_element_type=jnp.float32)
    return output.astype(jnp.bfloat16).reshape(rows_here, heads_here * HEAD_DIM), moved


def swap(array, axis, distance):
    count = lax.axis_size(axis)
    return lax.ppermute(array, axis, [(i, i ^ distance) for i in range(count)])


def ring_order(count):
    if count & (count - 1):
        return list(range(count))
    return [i ^ (i >> 1) for i in range(count)]


def turn(array, step):
    count = lax.axis_size("o")
    ring = ring_order(count)
    return lax.ppermute(
        array, "o", [(ring[i], ring[(i + step) % count]) for i in range(count)]
    )


def piece(array, index, size, dim):
    return lax.dynamic_slice_in_dim(array, index * size, size, dim)


def shards(
    queries,
    key_rows,
    values,
    sink_logit,
    residual_in,
    out_weight,
    norm_gain,
    gate_weight,
    up_weight,
    down_weight,
):
    rows_here = queries.shape[0]
    tp_count, group = lax.axis_size("tp"), lax.axis_size("q")
    row_share = rows_here // tp_count
    q_index, tp_index = lax.axis_index("q"), lax.axis_index("tp")
    units = gate_weight.shape[1] // group

    joined = jnp.concatenate([key_rows, values], axis=1)
    padded = with_halo(joined, ((("q", "o"), 0),), WINDOW)

    gate_up = jnp.stack([gate_weight, up_weight])
    gate_up_got, down_got = [], []
    for k in range(group):
        part = piece(gate_up, q_index ^ k, units, 2)
        gate_up_got.append(swap(part, "q", k) if k else part)
    for k in range(group):
        part = piece(down_weight, q_index ^ k, units, 0)
        down_got.append(swap(part, "q", k) if k else part)
    depth, width = gate_weight.shape[0], down_weight.shape[1]
    gate_up_mine = jnp.zeros((2, group * depth, units), gate_weight.dtype)
    down_mine = jnp.zeros((units, group * width), down_weight.dtype)
    for k in range(group):
        gate_up_mine = lax.dynamic_update_slice_in_dim(
            gate_up_mine, gate_up_got[k], (q_index ^ k) * depth, 1
        )
        down_mine = lax.dynamic_update_slice_in_dim(
            down_mine, down_got[k], (q_index ^ k) * width, 1
        )
    sp_index = lax.axis_index(("q", "o"))
    total_rows = rows_here * lax.axis_size(("q", "o"))
    mine = (gate_up_mine[0], gate_up_mine[1], down_mine)
    attended, mine = attend_window(
        queries, padded, sp_index * rows_here, total_rows, sink_logit, mine
    )
    outer = lax.axis_size("o")
    pieces = [(0, mine)]
    rings = [(x, x) for x in mine]
    if outer > 2:
        rings = [(turn(x, 1), turn(x, -1)) for x in mine]
        attended, rings[0] = lax.optimization_barrier((attended, rings[0]))

    partial_value = jnp.dot(attended, out_weight, preferred_element_type=jnp.float32).astype(
        jnp.bfloat16
    )
    mixed = residual_in.astype(jnp.float32) + piece(partial_value, tp_index, row_share, 0).astype(
        jnp.float32
    )
    for j in range(1, tp_count):
        sent = piece(partial_value, tp_index ^ j, row_share, 0)
        mixed = mixed + swap(sent, "tp", j).astype(jnp.float32)
    normed = rms_scale(mixed, norm_gain)
    normed = normed.reshape(row_share, group, outer, depth).swapaxes(1, 2).reshape(normed.shape)

    own = normed
    if outer > 2:
        own, rings[1] = lax.optimization_barrier((normed, rings[1]))
        pieces += [(-1, [x for x, _ in rings]), (1, [y for _, y in rings])]
    for distance in range(2, (outer - 1) // 2 + 1):
        rings = [(turn(x, 1), turn(y, -1)) for x, y in rings]
        pieces += [(-distance, [x for x, _ in rings]), (distance, [y for _, y in rings])]
    if outer > 1 and outer % 2 == 0:
        far = []
        for x, y in rings:
            half = x.shape[0] // 2
            far.append(jnp.concatenate([turn(x[:half], 1), turn(y[half:], -1)], axis=0))
        pieces.append((outer // 2, far))
    gate_full = jnp.zeros((outer * group * depth, units), gate_weight.dtype)
    up_full = jnp.zeros((outer * group * depth, units), gate_weight.dtype)
    down_full = jnp.zeros((units, outer * group * width), down_weight.dtype)
    for distance, (gate_part, up_part, down_part) in pieces:
        ring = ring_order(outer)
        inverse = [ring.index(i) for i in range(outer)]
        here = jnp.array(inverse, jnp.int32)[lax.axis_index("o")]
        place = jnp.array(ring, jnp.int32)[lax.rem(here + distance + outer, outer)]
        row = place * group * depth
        gate_full = lax.dynamic_update_slice_in_dim(gate_full, gate_part, row, 0)
        up_full = lax.dynamic_update_slice_in_dim(up_full, up_part, row, 0)
        down_full = lax.dynamic_update_slice_in_dim(down_full, down_part, place * group * width, 1)

    order = [*range(group - 1, 0, -1), 0]
    arrived = {k: swap(normed, "q", k) for k in order if k}
    arrived[0] = own
    result = jnp.zeros_like(mixed)
    waiting, received = None, []
    for k in order:
        rows = jnp.concatenate(
            [swap(arrived[k], "tp", j) if j else arrived[k] for j in range(tp_count)], axis=0
        )
        gate_pre = jnp.dot(rows, gate_full, preferred_element_type=jnp.float32)
        up_pre = jnp.dot(rows, up_full, preferred_element_type=jnp.float32)
        hidden = (jax.nn.silu(gate_pre) * up_pre).astype(jnp.bfloat16)
        if waiting is not None:
            sent, hidden = lax.optimization_barrier((waiting[1], hidden))
            received.append(swap(sent, "q", waiting[0]))
        if k == 0 and len(received) > 2:
            received[0], hidden = lax.optimization_barrier((received[0], hidden))
        parts = []
        for j in [*range(1, tp_count), 0]:
            if j == k == 0 and len(received) > 2:
                received[1], parts, hidden = lax.optimization_barrier(
                    (received[1], parts, hidden)
                )
            share = hidden[j * row_share : (j + 1) * row_share]
            out = jnp.dot(share, down_full, preferred_element_type=jnp.float32)
            out = out.astype(jnp.bfloat16)
            parts.append(swap(out, "tp", j) if j else out)
        total = sum(part.astype(jnp.float32) for part in parts)
        if k:
            waiting = (k, total.astype(jnp.bfloat16))
        else:
            result = result + total
    for part in received:
        result = result + part.astype(jnp.float32)
    result = result.reshape(row_share, outer, group, width).swapaxes(1, 2).reshape(mixed.shape)
    return (mixed + result).astype(jnp.bfloat16)


def solution(mesh):
    sp_count, tp_count = mesh.shape["sp"], mesh.shape["tp"]
    group = math.gcd(sp_count, 4)
    fine = Mesh(mesh.devices.reshape(group, sp_count // group, tp_count), ("q", "o", "tp"))
    sp = ("q", "o")
    return jax.shard_map(
        shards,
        mesh=fine,
        in_specs=(
            P(sp, "tp"),
            P(sp, "tp"),
            P(sp, "tp"),
            P("tp"),
            P(("q", "o", "tp"), None),
            P("tp", None),
            P(),
            P(sp, "tp"),
            P(sp, "tp"),
            P("tp", sp),
        ),
        out_specs=P(("q", "o", "tp"), None),
        check_vma=False,
    )
```
